32 devices in a mesh: ep: 8 (over z, core), tp: 4 (over y, x).
Axes of the slice: x: 2, y: 2, z: 4, core: 2. Of those that a mesh axis runs over, the one named last changes fastest.
Arguments:
- attn_rows: bfloat16 [1024, 2048], P('ep'), may hold values from -6 to 6
- attn_gain: float32 [2048], replicated, may hold values from 0.1 to 1.9
- query_weight: bfloat16 [2048, 1024], P(None, 'tp'), may hold values from -0.125 to 0.125
- key_weight: bfloat16 [2048, 1024], P(None, 'tp'), may hold values from -0.125 to 0.125
- value_weight: bfloat16 [2048, 1024], P(None, 'tp'), may hold values from -0.125 to 0.125
- key_bias: bfloat16 [16, 1024], P('tp', 'ep'), may hold values from -14 to 0
- out_weight: bfloat16 [1024, 2048], P(None, 'tp'), may hold values from -0.75 to 0.75
- expert_rows: bfloat16 [1024, 2048], P('ep'), may hold values from -6 to 6
- expert_gain: float32 [2048], replicated, may hold values from 0.1 to 1.9
- expert_ids: int32 [1024, 2], P('ep'), may hold values from 0 to 31, all different within a row; in each aligned block of 128 rows (0 to 127, 128 to 255, ...) at most 16 rows name the same one
- group_logits: float32 [1024, 4], P('ep'), may hold values from -6 to 6
- pair_logits: float32 [1024, 2], P('ep'), may hold values from -6 to 6
- gate_weight: bfloat16 [32, 2048, 2048], P('ep', None, 'tp'), may hold values from -0.125 to 0.125
- up_weight: bfloat16 [32, 2048, 2048], P('ep', None, 'tp'), may hold values from -0.125 to 0.125
- down_weight: bfloat16 [32, 2048, 2048], P('ep', None, 'tp'), may hold values from -0.125 to 0.125
Outputs:
- mixed: bfloat16 [1024, 2048], P('ep', 'tp')
- expert_out: bfloat16 [1024, 2048], P('ep', 'tp')
The draws below stay inside these ranges and needn't reach their ends.
Inputs may be any that keep to these rules, and one draw needn't show every extreme that they name: `expert_ids`: each row names two different experts; in every aligned block of 128 rows no expert is named more than 16 times.
All inputs are finite; a program needn't handle non-finite values.
Results may differ from the reference program's by a relative error of at most 0.0083.
Values may be sent and summed in bfloat16 or wider, within the bound.
A program may use at most 64 MiB of HBM per device.

```python
import math
import jax
import jax.numpy as jnp
import numpy as np
from jax import lax

D = 2048
ATTENTION_HEADS = 16
HEAD_DIM = 64
FF = 2048
EXPERTS = 32
GROUPS = 4
GROUP_SIZE = 8
TOK_DEV = 128
MICRO_TOKENS = 1024
CAP = 16
N_EP = 8


def draw_key_bias(key, part):
    parallel_lanes = jax.random.split(jax.random.fold_in(key, 17), 7)
    blocks = MICRO_TOKENS // TOK_DEV
    slow_share = 0.5
    slow = jax.random.uniform(parallel_lanes[0], (ATTENTION_HEADS, 1, 1)) < slow_share
    shift = jax.random.uniform(parallel_lanes[1], (ATTENTION_HEADS, blocks, 1), minval=-0.7, maxval=0.7)
    rough = 0.3 * jax.random.normal(parallel_lanes[2], (ATTENTION_HEADS, blocks, TOK_DEV))
    base = jnp.where(slow, -11.0, -4.2) + shift + rough
    spot = jax.random.randint(parallel_lanes[3], (ATTENTION_HEADS, blocks, 1), 0, TOK_DEV)
    strong = jax.random.uniform(parallel_lanes[4], (ATTENTION_HEADS, blocks, 1), minval=-4.0, maxval=-3.2)
    marked = jnp.arange(TOK_DEV)[None, None, :] == spot
    base = jnp.where(slow & marked, strong, base)
    flattened = base.reshape(ATTENTION_HEADS, MICRO_TOKENS)
    surge_position = jax.random.randint(parallel_lanes[5], (ATTENTION_HEADS, 2), 0, MICRO_TOKENS)
    surge_value = jax.random.uniform(parallel_lanes[6], (ATTENTION_HEADS, 2), minval=-1.4, maxval=-0.2)
    match_count = jnp.arange(MICRO_TOKENS)[None, None, :] == surge_position[:, :, None]
    surge_total_sum = jnp.sum(jnp.where(match_count, surge_value[:, :, None], 0.0), axis=1)
    flattened = jnp.where(jnp.any(match_count, axis=1), surge_total_sum, flattened)
    return jnp.clip(flattened, -14.0, 0.0).astype(jnp.float32).astype(jnp.bfloat16)


def block_levels(key, dims, cuts, least, largest):
    level, own = 1.0, jax.random.fold_in(key, 6)
    for dim, parts in cuts:
        heights = jnp.exp(jax.random.uniform(jax.random.fold_in(own, dim), (parts,), jnp.float32, least / len(cuts), largest / len(cuts)))
        level = level * jnp.repeat(heights, dims[dim] // parts).reshape([-1 if axis == dim else 1 for axis in range(len(dims))])
    return level


def assign_block(rng, own, number, rows, count, top, reach, slope):
    sequence = jax.random.permutation(rng, count)
    packed, common = load_shares(count, rows * top, reach, slope, True), load_shares(count, rows * top, reach, slope, False)
    places = jnp.arange(count)

    def named(lengths, turn):
        used = int((lengths > 0).sum())
        fixed = max(1, used // 4)
        moved = fixed + (places - fixed + turn * (used - fixed)) % max(1, count - fixed)
        return jnp.zeros((count,), jnp.int32).at[sequence[jnp.where(places < fixed, places, moved)]].set(jnp.asarray(lengths, jnp.int32))

    lengths = jnp.where(number % 4 == 0, named(packed, number // 4), named(common, number - number // 4 - 1))
    mixed = jax.random.permutation(jax.random.fold_in(own, 3), count)
    donor, sink = mixed[0:count // 2 * 2:2], mixed[1:count // 2 * 2:2]
    room = jnp.minimum(lengths[donor] - 1, reach - lengths[sink]) // 2
    room = jnp.where((donor == sequence[0]) | (sink == sequence[0]) | (lengths[sink] == 0), 0, jnp.maximum(room, 0))
    moved = jax.random.randint(jax.random.fold_in(own, 4), (count // 2,), 0, 1 << 20) % (room + 1)
    lengths = lengths.at[donor].add(-moved).at[sink].add(moved)
    labels = jnp.searchsorted(jnp.cumsum(lengths), jnp.arange(rows * top), side="right").astype(jnp.int32)
    table = labels.reshape(top, rows).T
    table = table[jax.random.permutation(jax.random.fold_in(own, 1), rows)]
    turn = jax.random.randint(jax.random.fold_in(own, 2), (rows, 1), 0, top)
    return jnp.take_along_axis(table, (jnp.arange(top)[None, :] + turn) % top, axis=1)


def load_shares(count, total, most, skew, full):
    portions = [(1 << 20) // math.isqrt(grade ** skew) + 1 for grade in range(1, count + 1)]
    largest = most if full else min(most, max(-(-total // count), total * portions[0] // sum(portions)))
    least = 1 if total - largest >= count - 1 else 0
    holding, spare = [largest] + [least] * (count - 1), total - largest - least * (count - 1)
    while spare > 0:
        free = [i for i in range(1, count) if holding[i] < largest] or [i for i in range(1, count) if holding[i] < most]
        whole, remaining = sum([portions[i] for i in free]), spare
        for i in free:
            addition = min(most - holding[i], max(1, remaining * portions[i] // whole), spare)
            holding[i] = holding[i] + addition
            spare = spare - addition
    return np.array(holding)


def gaussian(rng, extent, deviation, most, cuts=(), kind=jnp.bfloat16):
    values = deviation * jax.random.normal(rng, extent, jnp.float32)
    if cuts:
        values = values * block_levels(rng, extent, cuts, -0.22, 0.18)
    return jnp.clip(values, -most, most).astype(kind)


def setup_inputs(seed: int = 0) -> dict:
    arg_keys = jax.random.split(jax.random.key(seed), 16)
    attn_rows = gaussian(arg_keys[0], (MICRO_TOKENS, D), 1.0, 6.0, ((0, 8),))
    attn_gain = jnp.clip(1.0 + 0.18 * jax.random.normal(arg_keys[1], (D,), jnp.float32), 0.1, 1.9)
    query_weight = gaussian(arg_keys[2], (D, ATTENTION_HEADS * HEAD_DIM), D ** -0.5, 0.125, ((1, 4),))
    key_weight = gaussian(arg_keys[3], (D, ATTENTION_HEADS * HEAD_DIM), D ** -0.5, 0.125, ((1, 4),))
    value_weight = gaussian(arg_keys[4], (D, ATTENTION_HEADS * HEAD_DIM), D ** -0.5, 0.125, ((1, 4),))
    key_bias = draw_key_bias(jax.random.fold_in(arg_keys[15], 71), 0)
    out_weight = gaussian(arg_keys[6], (ATTENTION_HEADS * HEAD_DIM, D), (ATTENTION_HEADS * HEAD_DIM // 16) ** -0.5, 0.75, ((1, 4),))
    expert_rows = gaussian(arg_keys[7], (MICRO_TOKENS, D), 1.0, 6.0, ((0, 8),))
    expert_gain = jnp.clip(1.0 + 0.18 * jax.random.normal(arg_keys[8], (D,), jnp.float32), 0.1, 1.9)
    expert_ids_keys = jax.random.split(jax.random.fold_in(arg_keys[9], 1), MICRO_TOKENS // TOK_DEV)
    expert_ids_turns = jax.random.permutation(jax.random.fold_in(arg_keys[9], 3), MICRO_TOKENS // TOK_DEV)
    expert_ids = jax.vmap(lambda own, number: assign_block(jax.random.fold_in(arg_keys[9], 2), own, number, TOK_DEV, EXPERTS, 2, CAP, 2))(expert_ids_keys, expert_ids_turns).reshape((MICRO_TOKENS, 2))
    group_logits = gaussian(arg_keys[10], (MICRO_TOKENS, GROUPS), 1.5, 6.0, ((0, 8),), jnp.float32)
    pair_logits = gaussian(arg_keys[11], (MICRO_TOKENS, 2), 1.5, 6.0, ((0, 8),), jnp.float32)
    gate_weight = gaussian(arg_keys[12], (EXPERTS, D, FF), D ** -0.5, 0.125, ((0, 8), (2, 4)))
    up_weight = gaussian(arg_keys[13], (EXPERTS, D, FF), D ** -0.5, 0.125, ((0, 8), (2, 4)))
    down_weight = gaussian(arg_keys[14], (EXPERTS, FF, D), FF ** -0.5, 0.125, ((0, 8), (2, 4)))
    return {"attn_rows": attn_rows, "attn_gain": attn_gain, "query_weight": query_weight, "key_weight": key_weight, "value_weight": value_weight, "key_bias": key_bias, "out_weight": out_weight, "expert_rows": expert_rows, "expert_gain": expert_gain, "expert_ids": expert_ids, "group_logits": group_logits, "pair_logits": pair_logits, "gate_weight": gate_weight, "up_weight": up_weight, "down_weight": down_weight}


epsilon = 1e-06

def norm_rows(rows, gain):
    values = rows.astype(jnp.float32)
    scaled = values * lax.rsqrt(lax.optimization_barrier(jnp.mean(values * values, axis=-1, keepdims=True)) + epsilon)
    return (scaled * gain.astype(jnp.float32)).astype(jnp.bfloat16)

def attention_part(attn_rows, attn_gain, query_weight, key_weight, value_weight, key_bias, out_weight):
    normed = norm_rows(attn_rows, attn_gain)
    queries = jnp.dot(normed, query_weight, preferred_element_type=jnp.float32).astype(jnp.bfloat16)
    keys = jnp.dot(normed, key_weight, preferred_element_type=jnp.float32).astype(jnp.bfloat16)
    values = jnp.dot(normed, value_weight, preferred_element_type=jnp.float32).astype(jnp.bfloat16)
    q_blocks = queries.reshape(N_EP, TOK_DEV, ATTENTION_HEADS, HEAD_DIM).astype(jnp.float32)
    k_blocks = keys.reshape(N_EP, TOK_DEV, ATTENTION_HEADS, HEAD_DIM).astype(jnp.float32)
    v_blocks = values.reshape(N_EP, TOK_DEV, ATTENTION_HEADS, HEAD_DIM).astype(jnp.float32)
    bias_blocks = key_bias.astype(jnp.float32).reshape(ATTENTION_HEADS, N_EP, TOK_DEV)
    scale = HEAD_DIM ** (-0.5)
    local = jnp.arange(TOK_DEV, dtype=jnp.int32)

    def query_block(index):
        query = q_blocks[index]
        query_pos = index * TOK_DEV + local

        def key_block(carry, other):
            key_part = k_blocks[other]
            scores = jnp.einsum('thd,shd->hts', query, key_part) * scale + bias_blocks[:, other][:, None, :]
            causal = (other * TOK_DEV + local)[None, :] < query_pos[:, None]
            log_keep = jnp.where(causal, jax.nn.log_sigmoid(-scores), 0.0)
            suffix = lax.cumsum(log_keep, axis=2, reverse=True) - log_keep
            weights = jnp.where(causal, jnp.exp(jax.nn.log_sigmoid(scores) + suffix), 0.0).astype(jnp.bfloat16)
            block_out = jnp.einsum('hts,shd->htd', weights.astype(jnp.float32), v_blocks[other])
            return (carry, (lax.optimization_barrier(jnp.sum(log_keep, axis=2)), block_out))
        _, (totals, outputs) = lax.scan(key_block, jnp.zeros((), jnp.float32), jnp.arange(N_EP, dtype=jnp.int32))
        later = lax.cumsum(totals, axis=0, reverse=True) - totals
        merged = lax.optimization_barrier(jnp.sum(jnp.exp(later)[..., None] * outputs, axis=0))
        return jnp.transpose(merged, (1, 0, 2)).reshape(TOK_DEV, ATTENTION_HEADS * HEAD_DIM)
    attended = lax.map(query_block, jnp.arange(N_EP, dtype=jnp.int32))
    attended = attended.reshape(MICRO_TOKENS, ATTENTION_HEADS * HEAD_DIM).astype(jnp.bfloat16)
    return jnp.dot(attended, out_weight, preferred_element_type=jnp.float32).astype(jnp.bfloat16)

def route_shares(expert_ids, group_logits, pair_logits):
    shares = jnp.exp(group_logits)
    shares = shares / lax.optimization_barrier(jnp.sum(shares, axis=1, keepdims=True))
    groups = expert_ids // GROUP_SIZE
    marks = (groups[:, :, None] == jnp.arange(GROUPS, dtype=jnp.int32)[None, None, :]).astype(jnp.float32)
    chosen = lax.optimization_barrier(jnp.sum(shares[:, None, :] * marks, axis=2))
    spread = pair_logits[:, 0] - pair_logits[:, 1]
    pair_share = jnp.stack([jax.nn.sigmoid(spread), jax.nn.sigmoid(-spread)], axis=1)
    return chosen * pair_share

def expert_part(expert_rows, expert_gain, expert_ids, group_logits, pair_logits, gate_weight, up_weight, down_weight):
    normed = norm_rows(expert_rows, expert_gain)
    route_weights = route_shares(expert_ids, group_logits, pair_logits)
    flattened = expert_ids.astype(jnp.int32).reshape(N_EP, TOK_DEV * 2)
    marks = (flattened[:, :, None] == jnp.arange(EXPERTS, dtype=jnp.int32)[None, None, :]).astype(jnp.int32)
    position = lax.optimization_barrier(jnp.sum((jnp.cumsum(marks, axis=1) - marks) * marks, axis=2)).astype(jnp.int32)
    source = jnp.broadcast_to(jnp.arange(N_EP, dtype=jnp.int32)[:, None], flattened.shape)
    row_index = (jnp.arange(MICRO_TOKENS * 2, dtype=jnp.int32) // 2).astype(jnp.int32)
    flat_ids = flattened.reshape(-1)
    flat_src = source.reshape(-1)
    flat_pos = position.reshape(-1)
    buffer = jnp.zeros((EXPERTS, N_EP, CAP, D), jnp.bfloat16).at[flat_ids, flat_src, flat_pos].set(normed[row_index])

    def one_expert(args):
        rows, gate_w, up_w, down_w = args
        rows = rows.reshape(N_EP * CAP, D)
        gate = jnp.dot(rows, gate_w, preferred_element_type=jnp.float32)
        up = jnp.dot(rows, up_w, preferred_element_type=jnp.float32)
        hidden = (jax.nn.silu(gate) * up).astype(jnp.bfloat16)
        return jnp.dot(hidden, down_w, preferred_element_type=jnp.float32).astype(jnp.bfloat16)
    results = lax.map(one_expert, (buffer, gate_weight, up_weight, down_weight))
    picked = results[flat_ids, (flat_src * CAP + flat_pos).astype(jnp.int32)].reshape(MICRO_TOKENS, 2, D)
    combined = lax.optimization_barrier(jnp.sum(route_weights[:, :, None] * picked.astype(jnp.float32), axis=1))
    return combined.astype(jnp.bfloat16)

def reference(attn_rows, attn_gain, query_weight, key_weight, value_weight, key_bias, out_weight, expert_rows, expert_gain, expert_ids, group_logits, pair_logits, gate_weight, up_weight, down_weight):
    mixed = attention_part(attn_rows, attn_gain, query_weight, key_weight, value_weight, key_bias, out_weight)
    expert_out = expert_part(expert_rows, expert_gain, expert_ids, group_logits, pair_logits, gate_weight, up_weight, down_weight)
    return (mixed, expert_out)
```

```python
import functools

import jax
import jax.numpy as jnp
from jax import lax
from jax.experimental import pallas as pl
from jax.experimental.pallas import tpu as pltpu
from jax.sharding import PartitionSpec as P

MESH = pl.DeviceIdType.MESH
CAP = 16
GROUPS = 4
GROUP_SIZE = 8
BIAS_ROW = 8
epsilon = 1e-06
f32 = jnp.float32
bf16 = jnp.bfloat16


def dot(a, b):
    return jnp.dot(a, b, preferred_element_type=f32)


def loop(n, body, start=0):
    def step(i, carry):
        body(i)
        return carry

    lax.fori_loop(start, n, step, 0)


def kernel(
    E,
    T,
    rows_ref,
    again_ref,
    wq_hbm,
    wk_hbm,
    wv_hbm,
    meta_ref,
    wo_hbm,
    erows_hbm,
    egain_ref,
    ids_ref,
    glog_ref,
    plog_ref,
    wg_hbm,
    wu_hbm,
    wd_hbm,
    mixed_ref,
    out_ref,
    wqkv,
    wo,
    wg,
    wu,
    wd,
    X,
    XG,
    HB,
    M,
    KV,
    Q,
    AT,
    RES,
    RB,
    s_w,
    s_wg,
    s_wu,
    s_wd,
    s_lx,
    tx_z,
    tx_tp,
    tx_d,
    rx,
    tx_m,
    rx_m,
    tx_kv,
    tx_kvd,
    rx_kv,
    tx_h,
    rx_h,
    tx_a,
    rx_a,
    tx_r,
    rx_r,
):
    Z = E // 2
    R, D = rows_ref.shape
    W = wq_hbm.shape[1]
    DQ = X.shape[3]
    EL = wg.shape[0]
    FL = wg.shape[2]
    e = lax.axis_index("ep")
    t = lax.axis_index("tp")
    z = e // 2
    c = e % 2
    mate = 2 * z + (1 - c)
    HD = Q.shape[2]
    heads = Q.shape[0]
    scale = HD ** (-0.5)

    def remote(src, dst, ssem, rsem, de, dt):
        return pltpu.make_async_remote_copy(
            src_ref=src,
            dst_ref=dst,
            send_sem=ssem,
            recv_sem=rsem,
            device_id=(de, dt),
            device_id_type=MESH,
        )

    w_copies = [
        pltpu.make_async_copy(wk_hbm, wqkv.at[:, pl.ds(0, W)], s_w.at[0]),
        pltpu.make_async_copy(wv_hbm, wqkv.at[:, pl.ds(W, W)], s_w.at[1]),
        pltpu.make_async_copy(wq_hbm, wqkv.at[:, pl.ds(2 * W, W)], s_w.at[2]),
    ] if W % 128 == 0 else [
        pltpu.make_async_copy(wk_hbm, wqkv.at[0], s_w.at[0]),
        pltpu.make_async_copy(wv_hbm, wqkv.at[1], s_w.at[1]),
        pltpu.make_async_copy(wq_hbm, wqkv.at[2], s_w.at[2]),
    ]
    wo_copy = pltpu.make_async_copy(wo_hbm, wo, s_w.at[3])
    x_copies = [
        pltpu.make_async_copy(erows_hbm.at[:, pl.ds(q * DQ, DQ)], X.at[e, q], s_lx.at[q])
        for q in range(T)
    ]

    def wg_copy(i):
        return pltpu.make_async_copy(wg_hbm.at[i], wg.at[i], s_wg.at[i])

    def wu_copy(i):
        return pltpu.make_async_copy(wu_hbm.at[i], wu.at[i], s_wu.at[i])

    def wd_copy(i):
        return pltpu.make_async_copy(wd_hbm.at[i], wd.at[i], s_wd.at[i])

    for cp in x_copies + w_copies:
        cp.start()

    def start_gu(i):
        wg_copy(i).start()
        wu_copy(i).start()

    loop(EL, start_gu)
    loop(EL, lambda i: wd_copy(i).start())
    wo_copy.start()

    barrier = pltpu.get_barrier_semaphore()

    def greet_ep(d):
        pl.semaphore_signal(
            barrier, inc=1, device_id=((e + d) % E, t), device_id_type=MESH
        )

    def greet_tp(d):
        pl.semaphore_signal(
            barrier, inc=1, device_id=(e, (t + d) % T), device_id_type=MESH
        )

    loop(E, greet_ep, 1)
    loop(T, greet_tp, 1)
    pl.semaphore_wait(barrier, E - 1 + T - 1)

    for cp in x_copies:
        cp.wait()

    def z_copy(d):
        return remote(
            X.at[e, t], X.at[e, t], tx_z.at[d], rx.at[e, t], 2 * ((z + d) % Z) + c, t
        )

    def mate_copy(s, q):
        return remote(X.at[s, q], X.at[s, q], tx_d.at[s, q], rx.at[s, q], mate, t)

    def tp_copy(s, j):
        return remote(
            X.at[s, t], X.at[s, t], tx_tp.at[s, j], rx.at[s, t], e, (t + j) % T
        )

    def meta_copy(d):
        return remote(meta_ref, M.at[e], tx_m.at[d], rx_m.at[e], (e + d) % E, t)

    def kv_copy(d):
        return remote(
            KV.at[e], KV.at[e], tx_kv.at[d], rx_kv.at[e], 2 * ((z + d) % Z) + c, t
        )

    def kv_mate(s):
        return remote(KV.at[s], KV.at[s], tx_kvd.at[s], rx_kv.at[s], mate, t)

    def x_arrived(s, q):
        mate_copy(s, q).wait_recv()

    loop(E, lambda d: meta_copy(d).start(), 1)
    loop(Z, lambda d: z_copy(d).start(), 1)
    loop(T, lambda q: mate_copy(e, q).start())
    M[e] = meta_ref[...]

    values = rows_ref[...].astype(f32)
    scaled = values * lax.rsqrt(jnp.mean(values * values, axis=-1, keepdims=True) + epsilon)
    normed = (scaled * again_ref[...]).astype(bf16)
    for cp in w_copies:
        cp.wait()
    if W % 128 == 0:
        KV[e] = dot(normed, wqkv[:, : 2 * W]).astype(bf16)
    else:
        KV[e] = jnp.concatenate([dot(normed, wqkv[0]), dot(normed, wqkv[1])], axis=1).astype(bf16)

    def kv_send(d):
        @pl.when((z + d) % Z > z)
        def _():
            kv_copy(d).start()

    loop(Z, kv_send, 1)

    @pl.when(c == 0)
    def _():
        kv_mate(e).start()

    query = dot(normed, wqkv[:, 2 * W :] if W % 128 == 0 else wqkv[2]).astype(bf16)
    for h in range(heads):
        Q[h] = query[:, h * HD : (h + 1) * HD]

    def relay(d):
        s = 2 * ((z + d) % Z) + c
        x_arrived(s, t)
        loop(T, lambda j: tp_copy(s, j).start(), 1)
        mate_copy(s, t).start()

    loop(Z, relay, 1)

    row_i = lax.broadcasted_iota(jnp.int32, (R, R), 0)
    col_i = lax.broadcasted_iota(jnp.int32, (R, R), 1)
    before = (row_i < col_i).astype(f32).astype(bf16)
    after = (row_i > col_i).astype(f32).astype(bf16)
    slots = EL * CAP
    slot_i = lax.broadcasted_iota(jnp.int32, (slots, R), 0)
    slot_expert = (slot_i // CAP + e * EL).astype(f32)
    slot_place = (slot_i % CAP).astype(f32)

    def pick(s):
        names = M[s]
        mark = (names[0:1, :] == slot_expert) | (names[1:2, :] == slot_expert)
        place = dot(mark.astype(f32).astype(bf16), before)
        take = (mark & (place == slot_place)).astype(f32).astype(bf16)
        raw = [dot(take, X[s, q]) for q in range(T)]
        square = sum(jnp.sum(part * part, axis=1, keepdims=True) for part in raw)
        factor = lax.rsqrt(square / D + epsilon)
        for q in range(T):
            part = (raw[q] * factor * egain_ref[:, q * DQ : (q + 1) * DQ]).astype(bf16)
            for i in range(EL):
                XG[i, s, :, pl.ds(q * DQ, DQ)] = part[i * CAP : (i + 1) * CAP]

    loop(E, lambda d: remote(meta_ref, M.at[(e + d) % E], tx_m.at[0], rx_m.at[(e + d) % E], e, t).wait_recv(), 1)
    pick(e)

    def mate_rows(s):
        loop(T, lambda q: x_arrived(s, q))
        pick(s)

    mate_rows(mate)

    def kv_relay(s):
        kv_mate(s).wait_recv()
        kv_mate(s).start()

    loop(z, lambda k: kv_relay(2 * k + c))

    def spread(d):
        s = 2 * ((z + d) % Z) + c

        def on(j):
            q = (t + j) % T
            x_arrived(s, q)
            mate_copy(s, q).start()

        loop(T, on, 1)
        pick(s)

    loop(Z, spread, 1)
    loop(Z, lambda d: mate_rows(2 * ((z + d) % Z) + (1 - c)), 1)

    def h_copy(i, j):
        return remote(
            HB.at[t, i], HB.at[t, i], tx_h.at[i, j], rx_h.at[i, t], e, (t + j) % T
        )

    def hidden(i):
        rows = XG[i].reshape(E * CAP, D)
        wg_copy(i).wait()
        gate = dot(rows, wg[i])
        wu_copy(i).wait()
        up = dot(rows, wu[i])
        HB[t, i] = (jax.nn.silu(gate) * up).astype(bf16)
        loop(T, lambda j: h_copy(i, j).start(), 1)

    loop(EL, hidden)

    loop(z, lambda k: kv_mate(2 * k + (1 - c)).wait_recv())

    @pl.when(c == 1)
    def _():
        kv_mate(mate).wait_recv()

    def block(j, carry):
        s = e - j
        causal = col_i + s * R < row_i + e * R
        new = []
        for h in range(heads):
            later, total = carry[h]
            key = KV[s, :, pl.ds(h * HD, HD)]
            value = KV[s, :, pl.ds(W + h * HD, HD)]
            score = lax.dot_general(
                Q[h], key, (((1,), (1,)), ((), ())), preferred_element_type=f32
            )
            score = score * scale + M[s, pl.ds(BIAS_ROW + h, 1), :]
            negative = -(jnp.maximum(score, 0.0) + jnp.log1p(jnp.exp(-jnp.abs(score))))
            keep = jnp.where(causal, negative, 0.0)
            high = keep.astype(bf16)
            low = (keep - high.astype(f32)).astype(bf16)
            suffix = dot(high, after) + dot(low, after)
            weight = jnp.where(causal, jnp.exp(score + negative + suffix), 0.0).astype(bf16)
            total = total + jnp.exp(later) * dot(weight, value)
            later = later + suffix[:, 0:1] + keep[:, 0:1]
            new.append((later, total))
        return tuple(new)

    init = tuple(
        (jnp.zeros((R, 1), f32), jnp.zeros((R, HD), f32)) for _ in range(heads)
    )
    merged = lax.fori_loop(0, e + 1, block, init)
    AT[t] = jnp.concatenate([total for _, total in merged], axis=1).astype(bf16)

    def a_copy(j):
        return remote(AT.at[t], AT.at[t], tx_a.at[j], rx_a.at[t], e, (t + j) % T)

    loop(T, lambda j: a_copy(j).start(), 1)

    def r_copy(i, d):
        s = (e + d) % E
        return remote(RES.at[s, i], RB.at[e, i], tx_r.at[i, d], rx_r.at[e, i], s, t)

    def down(i):
        wd_copy(i).wait()

        def arrived(j):
            q = (t + j) % T
            remote(HB.at[q, i], HB.at[q, i], tx_h.at[i, 0], rx_h.at[i, q], e, t).wait_recv()

        loop(T, arrived, 1)
        result = dot(HB[0, i], wd[i, pl.ds(0, FL), :])
        for q in range(1, T):
            result = result + dot(HB[q, i], wd[i, pl.ds(q * FL, FL), :])
        result = result.astype(bf16).reshape(E, CAP, result.shape[1])
        RES[:, i] = result
        RB[e, i] = RES[e, i]
        loop(E, lambda d: r_copy(i, d).start(), 1)

    loop(EL, down)

    wo_copy.wait()

    def a_arrived(j):
        q = (t + j) % T
        remote(AT.at[q], AT.at[q], tx_a.at[0], rx_a.at[q], e, t).wait_recv()

    loop(T, a_arrived, 1)
    mixed = dot(AT[0], wo[pl.ds(0, W), :])
    for q in range(1, T):
        mixed = mixed + dot(AT[q], wo[pl.ds(q * W, W), :])
    mixed_ref[...] = mixed.astype(bf16)

    experts = E * EL
    ids = [ids_ref[:, k : k + 1] for k in range(2)]
    expert_i = lax.broadcasted_iota(jnp.int32, (R, experts), 1)
    named = (expert_i == ids[0]) | (expert_i == ids[1])
    places = dot(after, named.astype(f32).astype(bf16))
    shares = jnp.exp(glog_ref[...])
    shares = shares / jnp.sum(shares, axis=1, keepdims=True)
    group_i = lax.broadcasted_iota(jnp.int32, shares.shape, 1)
    back_i = lax.broadcasted_iota(jnp.int32, (R, experts * CAP), 1)
    pair = plog_ref[...]
    takes, shares_k = [], []
    for k in range(2):
        own = jnp.sum(jnp.where(expert_i == ids[k], places, 0.0), axis=1, keepdims=True)
        takes.append((back_i == ids[k] * CAP + own.astype(jnp.int32)).astype(f32).astype(bf16))
        chosen = jnp.sum(jnp.where(group_i == ids[k] // GROUP_SIZE, shares, 0.0), axis=1, keepdims=True)
        spread_k = pair[:, k : k + 1] - pair[:, 1 - k : 2 - k]
        shares_k.append(chosen * jax.nn.sigmoid(spread_k))

    def r_arrived(d):
        s = (e + d) % E
        for i in range(EL):
            remote(RES.at[s, i], RB.at[s, i], tx_r.at[i, 0], rx_r.at[s, i], s, t).wait_recv()

    loop(E, r_arrived, 1)
    returned = RB[...].reshape(experts * CAP, RB.shape[3])
    combined = shares_k[0] * dot(takes[0], returned) + shares_k[1] * dot(takes[1], returned)
    out_ref[...] = combined.astype(bf16)

    loop(E, lambda d: meta_copy(d).wait_send(), 1)
    loop(Z, lambda d: z_copy(d).wait_send(), 1)
    loop(T, lambda q: mate_copy(e, q).wait_send())

    def sent(d):
        s = 2 * ((z + d) % Z) + c
        loop(T, lambda j: tp_copy(s, j).wait_send(), 1)
        loop(T, lambda q: mate_copy(s, q).wait_send())

        @pl.when((z + d) % Z > z)
        def _():
            kv_copy(d).wait_send()

    loop(Z, sent, 1)
    loop(z, lambda k: kv_mate(2 * k + c).wait_send())

    @pl.when(c == 0)
    def _():
        kv_mate(e).wait_send()

    def sent_expert(i):
        loop(T, lambda j: h_copy(i, j).wait_send(), 1)
        loop(E, lambda d: r_copy(i, d).wait_send(), 1)

    loop(EL, sent_expert)
    loop(T, lambda j: a_copy(j).wait_send(), 1)


def shards(
    E,
    T,
    attn_rows,
    attn_gain,
    query_weight,
    key_weight,
    value_weight,
    key_bias,
    out_weight,
    expert_rows,
    expert_gain,
    expert_ids,
    group_logits,
    pair_logits,
    gate_weight,
    up_weight,
    down_weight,
):
    R, D = attn_rows.shape
    W = query_weight.shape[1]
    heads = key_bias.shape[0]
    HD = W // heads
    EL, _, FL = gate_weight.shape
    DL = down_weight.shape[2]
    Z = E // 2
    DQ = D // T
    meta_rows = BIAS_ROW + -(-heads // 8) * 8
    meta = jnp.concatenate(
        [
            jnp.pad(expert_ids.T.astype(f32), ((0, BIAS_ROW - 2), (0, 0))),
            jnp.pad(key_bias.astype(f32), ((0, meta_rows - BIAS_ROW - heads), (0, 0))),
        ],
        axis=0,
    )
    vmem = pl.BlockSpec(memory_space=pltpu.VMEM)
    hbm = pl.BlockSpec(memory_space=pl.ANY)
    dma = pltpu.SemaphoreType.DMA
    qkv = (D, 3 * W) if W % 128 == 0 else (3, D, W)
    return pl.pallas_call(
        functools.partial(kernel, E, T),
        out_shape=(
            jax.ShapeDtypeStruct((R, out_weight.shape[1]), bf16),
            jax.ShapeDtypeStruct((R, DL), bf16),
        ),
        in_specs=[vmem, vmem, hbm, hbm, hbm, vmem, hbm, hbm, vmem, vmem, vmem, vmem, hbm, hbm, hbm],
        out_specs=(vmem, vmem),
        scratch_shapes=[
            pltpu.VMEM(qkv, bf16),
            pltpu.VMEM(out_weight.shape, bf16),
            pltpu.VMEM(gate_weight.shape, bf16),
            pltpu.VMEM(up_weight.shape, bf16),
            pltpu.VMEM(down_weight.shape, bf16),
            pltpu.VMEM((E, T, R, DQ), bf16),
            pltpu.VMEM((EL, E, CAP, D), bf16),
            pltpu.VMEM((T, EL, E * CAP, FL), bf16),
            pltpu.VMEM((E, meta_rows, R), f32),
            pltpu.VMEM((E, R, 2 * W), bf16),
            pltpu.VMEM((heads, R, HD), bf16),
            pltpu.VMEM((T, R, W), bf16),
            pltpu.VMEM((E, EL, CAP, DL), bf16),
            pltpu.VMEM((E, EL, CAP, DL), bf16),
            dma((4,)),
            dma((EL,)),
            dma((EL,)),
            dma((EL,)),
            dma((T,)),
            dma((Z,)),
            dma((E, T)),
            dma((E, T)),
            dma((E, T)),
            dma((E,)),
            dma((E,)),
            dma((Z,)),
            dma((E,)),
            dma((E,)),
            dma((EL, T)),
            dma((EL, T)),
            dma((T,)),
            dma((T,)),
            dma((EL, E)),
            dma((E, EL)),
        ],
        compiler_params=pltpu.CompilerParams(
            collective_id=0, has_side_effects=True, vmem_limit_bytes=63 * 1024 * 1024
        ),
    )(
        attn_rows,
        attn_gain.reshape(1, D),
        query_weight,
        key_weight,
        value_weight,
        meta,
        out_weight,
        expert_rows,
        expert_gain.reshape(1, D),
        expert_ids,
        group_logits,
        pair_logits,
        gate_weight,
        up_weight,
        down_weight,
    )


def solution(mesh):
    placed = (
        P("ep", None),
        P(),
        P(None, "tp"),
        P(None, "tp"),
        P(None, "tp"),
        P("tp", "ep"),
        P(None, "tp"),
        P("ep", None),
        P(),
        P("ep", None),
        P("ep", None),
        P("ep", None),
        P("ep", None, "tp"),
        P("ep", None, "tp"),
        P("ep", None, "tp"),
    )
    return jax.shard_map(
        functools.partial(shards, mesh.shape["ep"], mesh.shape["tp"]),
        mesh=mesh,
        in_specs=placed,
        out_specs=(P("ep", "tp"), P("ep", "tp")),
        check_vma=False,
    )
```

```python
import functools

import jax
import jax.numpy as jnp
from jax import lax
from jax.experimental import pallas as pl
from jax.experimental.pallas import tpu as pltpu
from jax.sharding import PartitionSpec as P

MESH = pl.DeviceIdType.MESH
CAP = 16
GROUPS = 4
GROUP_SIZE = 8
BIAS_ROW = 8
epsilon = 1e-06
f32 = jnp.float32
bf16 = jnp.bfloat16


def dot(a, b):
    return jnp.dot(a, b, preferred_element_type=f32)


def loop(n, body, start=0):
    def step(i, carry):
        body(i)
        return carry

    lax.fori_loop(start, n, step, 0)


def kernel(
    E,
    T,
    rows_ref,
    again_ref,
    wq_hbm,
    wk_hbm,
    wv_hbm,
    bias_ref,
    wo_hbm,
    erows_hbm,
    egain_ref,
    ids_ref,
    glog_ref,
    plog_ref,
    wg_hbm,
    wu_hbm,
    wd_hbm,
    mixed_ref,
    out_ref,
    wqkv,
    wo,
    wg,
    wu,
    wd,
    X,
    XG,
    HB,
    M,
    KV,
    Q,
    AT,
    RES,
    RB,
    COL,
    s_w,
    s_wg,
    s_wu,
    s_wd,
    s_lx,
    tx_z,
    tx_tp,
    tx_d,
    rx,
    tx_m,
    rx_m,
    tx_kv,
    tx_kvd,
    rx_kv,
    tx_h,
    rx_h,
    tx_a,
    rx_a,
    tx_r,
    rx_r,
    tx_f,
    rx_f,
    tx_hf,
    rx_hf,
):
    square = T == 4
    Z = E // 2
    R, D = rows_ref.shape
    W = wq_hbm.shape[1]
    DQ = X.shape[3]
    EL = wg.shape[0]
    FL = wg.shape[2]
    e = lax.axis_index("ep")
    t = lax.axis_index("tp")
    z = e // 2
    c = e % 2
    mate = 2 * z + (1 - c)
    HD = Q.shape[2]
    heads = Q.shape[0]
    scale = HD ** (-0.5)

    def remote(src, dst, ssem, rsem, de, dt):
        return pltpu.make_async_remote_copy(
            src_ref=src,
            dst_ref=dst,
            send_sem=ssem,
            recv_sem=rsem,
            device_id=(de, dt),
            device_id_type=MESH,
        )

    w_copies = [
        pltpu.make_async_copy(wk_hbm, wqkv.at[:, pl.ds(0, W)], s_w.at[0]),
        pltpu.make_async_copy(wv_hbm, wqkv.at[:, pl.ds(W, W)], s_w.at[1]),
        pltpu.make_async_copy(wq_hbm, wqkv.at[:, pl.ds(2 * W, W)], s_w.at[2]),
    ] if W % 128 == 0 else [
        pltpu.make_async_copy(wk_hbm, wqkv.at[0], s_w.at[0]),
        pltpu.make_async_copy(wv_hbm, wqkv.at[1], s_w.at[1]),
        pltpu.make_async_copy(wq_hbm, wqkv.at[2], s_w.at[2]),
    ]
    wo_copy = pltpu.make_async_copy(wo_hbm, wo, s_w.at[3])
    x_copies = [
        pltpu.make_async_copy(erows_hbm.at[:, pl.ds(q * DQ, DQ)], X.at[e, q], s_lx.at[q])
        for q in range(T)
    ]

    def wg_copy(i):
        return pltpu.make_async_copy(wg_hbm.at[i], wg.at[i], s_wg.at[i])

    def wu_copy(i):
        return pltpu.make_async_copy(wu_hbm.at[i], wu.at[i], s_wu.at[i])

    def wd_copy(i):
        return pltpu.make_async_copy(wd_hbm.at[i], wd.at[i], s_wd.at[i])

    for cp in x_copies + w_copies:
        cp.start()

    def start_gu(i):
        wg_copy(i).start()
        wu_copy(i).start()

    loop(EL, start_gu)
    loop(EL, lambda i: wd_copy(i).start())
    wo_copy.start()

    barrier = pltpu.get_barrier_semaphore()

    def greet_ep(d):
        pl.semaphore_signal(
            barrier, inc=1, device_id=((e + d) % E, t), device_id_type=MESH
        )

    def greet_tp(d):
        pl.semaphore_signal(
            barrier, inc=1, device_id=(e, (t + d) % T), device_id_type=MESH
        )

    loop(E, greet_ep, 1)
    loop(T, greet_tp, 1)
    pl.semaphore_wait(barrier, E - 1 + T - 1)

    M[e] = jnp.zeros(M.shape[1:], f32)
    M[e, 0:2, :] = ids_ref[...].astype(f32)
    M[e, BIAS_ROW : BIAS_ROW + heads, :] = bias_ref[...].astype(f32)

    for cp in x_copies:
        cp.wait()

    def z_copy(d):
        return remote(
            X.at[e, t], X.at[e, t], tx_z.at[d], rx.at[e, t], 2 * ((z + d) % Z) + c, t
        )

    def mate_copy(s, q):
        return remote(X.at[s, q], X.at[s, q], tx_d.at[s, q], rx.at[s, q], mate, t)

    side, down_side, far = t - t % 2 + 1 - t % 2, (t + 2) % 4, 3 - t
    peers = [side, down_side] if square else [(t + j) % T for j in range(1, T)]
    half = R // 2

    def to_peers(make):
        for j, peer in enumerate(peers):
            make(j, peer)

    def tp_copy(s, j, peer):
        return remote(X.at[s, t], X.at[s, t], tx_tp.at[s, j], rx.at[s, t], e, peer)

    def pass_first(s):
        part = X.at[s, side, pl.ds(0, half)]
        return remote(part, part, tx_f.at[s, 0], rx.at[s, side], e, down_side)

    def pass_second(s):
        part = X.at[s, down_side, pl.ds(half, R - half)]
        return remote(part, part, tx_f.at[s, 1], rx_f.at[s], e, side)

    def far_arrived(s):
        part = X.at[s, far, pl.ds(0, half)]
        remote(part, part, tx_f.at[s, 0], rx.at[s, far], e, t).wait_recv()
        part = X.at[s, far, pl.ds(half, R - half)]
        remote(part, part, tx_f.at[s, 1], rx_f.at[s], e, t).wait_recv()

    def meta_copy(d):
        return remote(M.at[e], M.at[e], tx_m.at[d], rx_m.at[e], (e + d) % E, t)

    def kv_copy(d):
        return remote(
            KV.at[e], KV.at[e], tx_kv.at[d], rx_kv.at[e], 2 * ((z + d) % Z) + c, t
        )

    def kv_mate(s):
        return remote(KV.at[s], KV.at[s], tx_kvd.at[s], rx_kv.at[s], mate, t)

    def x_arrived(s, q):
        mate_copy(s, q).wait_recv()

    loop(Z, lambda d: z_copy(d).start(), 1)
    loop(E, lambda d: meta_copy(d).start(), 1)
    loop(T, lambda q: mate_copy(e, q).start())

    values = rows_ref[...].astype(f32)
    scaled = values * lax.rsqrt(jnp.mean(values * values, axis=-1, keepdims=True) + epsilon)
    normed = (scaled * again_ref[...]).astype(bf16)
    for cp in w_copies:
        cp.wait()
    if W % 128 == 0:
        KV[e] = dot(normed, wqkv[:, : 2 * W]).astype(bf16)
    else:
        KV[e] = jnp.concatenate([dot(normed, wqkv[0]), dot(normed, wqkv[1])], axis=1).astype(bf16)

    query = dot(normed, wqkv[:, 2 * W :] if W % 128 == 0 else wqkv[2]).astype(bf16)
    for h in range(heads):
        Q[h] = query[:, h * HD : (h + 1) * HD]

    def relay(d):
        s = 2 * ((z + d) % Z) + c
        x_arrived(s, t)
        to_peers(lambda j, peer: tp_copy(s, j, peer).start())
        mate_copy(s, t).start()

    loop(Z, relay, 1)

    def kv_send(d):
        @pl.when((z + d) % Z > z)
        def _():
            kv_copy(d).start()

    loop(Z, kv_send, 1)

    @pl.when(c == 0)
    def _():
        kv_mate(e).start()


    row_i = lax.broadcasted_iota(jnp.int32, (R, R), 0)
    col_i = lax.broadcasted_iota(jnp.int32, (R, R), 1)
    before = (row_i < col_i).astype(f32).astype(bf16)
    after = (row_i > col_i).astype(f32).astype(bf16)
    slots = EL * CAP
    slot_i = lax.broadcasted_iota(jnp.int32, (slots, R), 0)
    slot_expert = (slot_i // CAP + e * EL).astype(f32)
    slot_place = (slot_i % CAP).astype(f32)

    def pick(s):
        names = M[s]
        mark = (names[0:1, :] == slot_expert) | (names[1:2, :] == slot_expert)
        place = dot(mark.astype(f32).astype(bf16), before)
        take = (mark & (place == slot_place)).astype(f32).astype(bf16)
        raw = [dot(take, X[s, q]) for q in range(T)]
        square = sum(jnp.sum(part * part, axis=1, keepdims=True) for part in raw)
        factor = lax.rsqrt(square / D + epsilon)
        for q in range(T):
            part = (raw[q] * factor * egain_ref[:, q * DQ : (q + 1) * DQ]).astype(bf16)
            for i in range(EL):
                XG[i, s, :, pl.ds(q * DQ, DQ)] = part[i * CAP : (i + 1) * CAP]

    loop(E, lambda d: remote(M.at[(e + d) % E], M.at[(e + d) % E], tx_m.at[0], rx_m.at[(e + d) % E], e, t).wait_recv(), 1)
    pick(e)

    def mate_rows(s):
        loop(T, lambda q: x_arrived(s, q))
        pick(s)

    def kv_relay(s):
        kv_mate(s).wait_recv()
        kv_mate(s).start()

    if square:

        def forward(d):
            s = 2 * ((z + d) % Z) + c
            x_arrived(s, side)
            pass_first(s).start()
            mate_copy(s, side).start()
            x_arrived(s, down_side)
            pass_second(s).start()
            mate_copy(s, down_side).start()

        loop(Z, forward, 1)

    mate_rows(mate)
    loop(z, lambda k: kv_relay(2 * k + c))

    def spread(d):
        s = 2 * ((z + d) % Z) + c
        if square:
            far_arrived(s)
            mate_copy(s, far).start()
        else:
            for q in peers:
                x_arrived(s, q)
                mate_copy(s, q).start()
        pick(s)

    loop(Z, spread, 1)
    loop(Z, lambda d: mate_rows(2 * ((z + d) % Z) + (1 - c)), 1)

    def h_copy(i, j, peer):
        return remote(HB.at[t, i], HB.at[t, i], tx_h.at[i, j], rx_h.at[i, t], e, peer)

    def h_arrived(i, q):
        remote(HB.at[q, i], HB.at[q, i], tx_h.at[i, 0], rx_h.at[i, q], e, t).wait_recv()

    h_half = E * CAP // 2

    def h_first(i, q, peer):
        part = HB.at[q, i, pl.ds(0, h_half)]
        return remote(part, part, tx_hf.at[i, 0], rx_h.at[i, q], e, peer)

    def h_second(i, q, peer):
        part = HB.at[q, i, pl.ds(h_half, h_half)]
        return remote(part, part, tx_hf.at[i, 1], rx_hf.at[i], e, peer)

    def h_forward(i):
        h_arrived(i, side)
        h_first(i, side, down_side).start()
        h_arrived(i, down_side)
        h_second(i, down_side, side).start()

    def hidden(i):
        rows = XG[i].reshape(E * CAP, D)
        wg_copy(i).wait()
        gate = dot(rows, wg[i])
        wu_copy(i).wait()
        up = dot(rows, wu[i])
        HB[t, i] = (jax.nn.silu(gate) * up).astype(bf16)
        to_peers(lambda j, peer: h_copy(i, j, peer).start())

    for i in range(EL):
        hidden(i)
        if square and i >= 2:
            h_forward(i - 2)

    loop(z, lambda k: kv_mate(2 * k + (1 - c)).wait_recv())

    @pl.when(c == 1)
    def _():
        kv_mate(mate).wait_recv()

    def attend(group):
        def block(j, carry):
            s = e - j
            causal = col_i + s * R < row_i + e * R
            new = []
            for h, (later, total) in zip(group, carry):
                key = KV[s, :, pl.ds(h * HD, HD)]
                value = KV[s, :, pl.ds(W + h * HD, HD)]
                score = lax.dot_general(
                    Q[h], key, (((1,), (1,)), ((), ())), preferred_element_type=f32
                )
                score = score * scale + M[s, pl.ds(BIAS_ROW + h, 1), :]
                negative = -(jnp.maximum(score, 0.0) + jnp.log1p(jnp.exp(-jnp.abs(score))))
                keep = jnp.where(causal, negative, 0.0)
                high = keep.astype(bf16)
                low = (keep - high.astype(f32)).astype(bf16)
                suffix = dot(high, after) + dot(low, after)
                weight = jnp.where(causal, jnp.exp(score + negative + suffix), 0.0).astype(bf16)
                total = total + jnp.exp(later) * dot(weight, value)
                later = later + suffix[:, 0:1] + keep[:, 0:1]
                new.append((later, total))
            return tuple(new)

        init = tuple((jnp.zeros((R, 1), f32), jnp.zeros((R, HD), f32)) for _ in group)
        return [total for _, total in lax.fori_loop(0, e + 1, block, init)]

    attended = []
    late = list(range(max(EL - 2, 0), EL)) if square else []
    for first in range(0, heads, 2):
        attended += attend(list(range(first, min(first + 2, heads))))
        if late:
            h_forward(late.pop(0))
    for i in late:
        h_forward(i)
    AT[t] = jnp.concatenate(attended, axis=1).astype(bf16)

    def a_copy(j):
        return remote(AT.at[t], AT.at[t], tx_a.at[j], rx_a.at[t], e, (t + j) % T)

    loop(T, lambda j: a_copy(j).start(), 1)

    def r_copy(i, d):
        s = (e + d) % E
        return remote(RES.at[s, i], RB.at[e, i], tx_r.at[i, d], rx_r.at[e, i], s, t)

    def down(i):
        wd_copy(i).wait()

        if square:
            h_first(i, far, t).wait_recv()
            h_second(i, far, t).wait_recv()
        else:
            for q in peers:
                h_arrived(i, q)
        result = dot(HB[0, i], wd[i, pl.ds(0, FL), :])
        for q in range(1, T):
            result = result + dot(HB[q, i], wd[i, pl.ds(q * FL, FL), :])
        result = result.astype(bf16).reshape(E, CAP, result.shape[1])
        RES[:, i] = result
        RB[e, i] = RES[e, i]
        loop(E, lambda d: r_copy(i, d).start(), 1)

    loop(EL, down)

    wo_copy.wait()

    def a_arrived(j):
        q = (t + j) % T
        remote(AT.at[q], AT.at[q], tx_a.at[0], rx_a.at[q], e, t).wait_recv()

    loop(T, a_arrived, 1)
    mixed = dot(AT[0], wo[pl.ds(0, W), :])
    for q in range(1, T):
        mixed = mixed + dot(AT[q], wo[pl.ds(q * W, W), :])
    mixed_ref[...] = mixed.astype(bf16)

    experts = E * EL
    groups = glog_ref.shape[0]
    COL[...] = jnp.zeros(COL.shape, f32)
    COL[0:2, :] = ids_ref[...].astype(f32)
    COL[2 : 2 + groups, :] = glog_ref[...]
    COL[2 + groups : 4 + groups, :] = plog_ref[...]
    columns = COL[...].T
    ids = [columns[:, k : k + 1].astype(jnp.int32) for k in range(2)]
    expert_i = lax.broadcasted_iota(jnp.int32, (R, experts), 1)
    named = (expert_i == ids[0]) | (expert_i == ids[1])
    places = dot(after, named.astype(f32).astype(bf16))
    shares = jnp.exp(columns[:, 2 : 2 + groups])
    shares = shares / jnp.sum(shares, axis=1, keepdims=True)
    group_i = lax.broadcasted_iota(jnp.int32, shares.shape, 1)
    back_i = lax.broadcasted_iota(jnp.int32, (R, experts * CAP), 1)
    pair = columns[:, 2 + groups : 4 + groups]
    takes, shares_k = [], []
    for k in range(2):
        own = jnp.sum(jnp.where(expert_i == ids[k], places, 0.0), axis=1, keepdims=True)
        takes.append((back_i == ids[k] * CAP + own.astype(jnp.int32)).astype(f32).astype(bf16))
        chosen = jnp.sum(jnp.where(group_i == ids[k] // GROUP_SIZE, shares, 0.0), axis=1, keepdims=True)
        spread_k = pair[:, k : k + 1] - pair[:, 1 - k : 2 - k]
        shares_k.append(chosen * jax.nn.sigmoid(spread_k))

    def r_arrived(d):
        s = (e + d) % E
        for i in range(EL):
            remote(RES.at[s, i], RB.at[s, i], tx_r.at[i, 0], rx_r.at[s, i], s, t).wait_recv()

    loop(E, r_arrived, 1)
    returned = RB[...].reshape(experts * CAP, RB.shape[3])
    combined = shares_k[0] * dot(takes[0], returned) + shares_k[1] * dot(takes[1], returned)
    out_ref[...] = combined.astype(bf16)

    loop(E, lambda d: meta_copy(d).wait_send(), 1)
    loop(Z, lambda d: z_copy(d).wait_send(), 1)
    loop(T, lambda q: mate_copy(e, q).wait_send())

    def sent(d):
        s = 2 * ((z + d) % Z) + c
        to_peers(lambda j, peer: tp_copy(s, j, peer).wait_send())
        if square:
            pass_first(s).wait_send()
            pass_second(s).wait_send()
        loop(T, lambda q: mate_copy(s, q).wait_send())

        @pl.when((z + d) % Z > z)
        def _():
            kv_copy(d).wait_send()

    loop(Z, sent, 1)
    loop(z, lambda k: kv_mate(2 * k + c).wait_send())

    @pl.when(c == 0)
    def _():
        kv_mate(e).wait_send()

    def sent_expert(i):
        to_peers(lambda j, peer: h_copy(i, j, peer).wait_send())
        if square:
            h_first(i, side, down_side).wait_send()
            h_second(i, down_side, side).wait_send()
        loop(E, lambda d: r_copy(i, d).wait_send(), 1)

    loop(EL, sent_expert)
    loop(T, lambda j: a_copy(j).wait_send(), 1)


def write_results(mixed_ref, out_ref, mixed_to, out_to):
    mixed_to[...] = mixed_ref[...]
    out_to[...] = out_ref[...]


def shards(
    E,
    T,
    attn_rows,
    attn_gain,
    query_weight,
    key_weight,
    value_weight,
    key_bias,
    out_weight,
    expert_rows,
    expert_gain,
    expert_ids,
    group_logits,
    pair_logits,
    gate_weight,
    up_weight,
    down_weight,
):
    R, D = attn_rows.shape
    W = query_weight.shape[1]
    heads = key_bias.shape[0]
    HD = W // heads
    EL, _, FL = gate_weight.shape
    DL = down_weight.shape[2]
    Z = E // 2
    DQ = D // T
    meta_rows = BIAS_ROW + -(-heads // 8) * 8
    col_rows = -(-(4 + group_logits.shape[1]) // 8) * 8
    vmem = pl.BlockSpec(memory_space=pltpu.VMEM)
    hbm = pl.BlockSpec(memory_space=pl.ANY)
    dma = pltpu.SemaphoreType.DMA
    qkv = (D, 3 * W) if W % 128 == 0 else (3, D, W)
    results = pl.pallas_call(
        functools.partial(kernel, E, T),
        out_shape=(
            jax.ShapeDtypeStruct((R, out_weight.shape[1]), bf16),
            jax.ShapeDtypeStruct((R, DL), bf16),
        ),
        in_specs=[vmem, vmem, hbm, hbm, hbm, vmem, hbm, hbm, vmem, vmem, vmem, vmem, hbm, hbm, hbm],
        out_specs=(vmem, vmem),
        scratch_shapes=[
            pltpu.VMEM(qkv, bf16),
            pltpu.VMEM(out_weight.shape, bf16),
            pltpu.VMEM(gate_weight.shape, bf16),
            pltpu.VMEM(up_weight.shape, bf16),
            pltpu.VMEM(down_weight.shape, bf16),
            pltpu.VMEM((E, T, R, DQ), bf16),
            pltpu.VMEM((EL, E, CAP, D), bf16),
            pltpu.VMEM((T, EL, E * CAP, FL), bf16),
            pltpu.VMEM((E, meta_rows, R), f32),
            pltpu.VMEM((E, R, 2 * W), bf16),
            pltpu.VMEM((heads, R, HD), bf16),
            pltpu.VMEM((T, R, W), bf16),
            pltpu.VMEM((E, EL, CAP, DL), bf16),
            pltpu.VMEM((E, EL, CAP, DL), bf16),
            pltpu.VMEM((col_rows, R), f32),
            dma((4,)),
            dma((EL,)),
            dma((EL,)),
            dma((EL,)),
            dma((T,)),
            dma((Z,)),
            dma((E, T)),
            dma((E, T)),
            dma((E, T)),
            dma((E,)),
            dma((E,)),
            dma((Z,)),
            dma((E,)),
            dma((E,)),
            dma((EL, T)),
            dma((EL, T)),
            dma((T,)),
            dma((T,)),
            dma((EL, E)),
            dma((E, EL)),
            dma((E, 2)),
            dma((E,)),
            dma((EL, 2)),
            dma((EL,)),
        ],
        compiler_params=pltpu.CompilerParams(
            collective_id=0, has_side_effects=True, vmem_limit_bytes=63 * 1024 * 1024
        ),
    )(
        attn_rows,
        attn_gain.reshape(1, D),
        query_weight,
        key_weight,
        value_weight,
        key_bias,
        out_weight,
        expert_rows,
        expert_gain.reshape(1, D),
        expert_ids.T,
        group_logits.T,
        pair_logits.T,
        gate_weight,
        up_weight,
        down_weight,
    )
    return pl.pallas_call(
        write_results,
        out_shape=tuple(jax.ShapeDtypeStruct(r.shape, r.dtype) for r in results),
        in_specs=[vmem, vmem],
        out_specs=(vmem, vmem),
    )(*results)


def solution(mesh):
    placed = (
        P("ep", None),
        P(),
        P(None, "tp"),
        P(None, "tp"),
        P(None, "tp"),
        P("tp", "ep"),
        P(None, "tp"),
        P("ep", None),
        P(),
        P("ep", None),
        P("ep", None),
        P("ep", None),
        P("ep", None, "tp"),
        P("ep", None, "tp"),
        P("ep", None, "tp"),
    )
    return jax.shard_map(
        functools.partial(shards, mesh.shape["ep"], mesh.shape["tp"]),
        mesh=mesh,
        in_specs=placed,
        out_specs=(P("ep", "tp"), P("ep", "tp")),
        check_vma=False,
    )
```
